128 devices in a mesh: gr: 2 (over z_hi), sp: 32 (over z_lo, y, x), tp: 2 (over core).
Axes of the slice: x: 4, y: 4, z: 4 (z_hi: 2, z_lo: 2; z = z_hi * 2 + z_lo), core: 2. Of those that a mesh axis runs over, the one named last changes fastest.
Arguments:
- tokens: bfloat16 [2, 2, 24576, 2048], P('gr', 'tp', 'sp'), may hold values from -6 to 6
- key_weight: bfloat16 [2048, 2048], replicated, may hold values from -0.125 to 0.125
- value_weight: bfloat16 [2048, 2048], replicated, may hold values from -0.125 to 0.125
- cum_gate: float32 [2, 32, 2, 24576], P('gr', None, 'tp', 'sp'), may hold values from -49452 to 0, as said below
- query: bfloat16 [2, 32, 64], P('gr', 'sp'), may hold values from -12 to 12
Outputs:
- kv_cache: bfloat16 [2, 32, 49152, 128], P('gr', 'sp', 'tp')
- gate_cache: float32 [2, 32, 49152], P('gr', 'sp', 'tp')
- read: bfloat16 [2, 32, 64], P('gr', 'sp')
The draws below stay inside these ranges and needn't reach their ends.
Inputs may be any that keep to these rules, and one draw needn't show every extreme that they name: `cum_gate`: each head's entries never rise along the positions.
All inputs are finite; a program needn't handle non-finite values.
Results may differ from the reference program's by a relative error of at most 0.012.
Values may be sent and summed in bfloat16 or wider, within the bound.
A program may use at most 128 MiB of HBM per device.

```python
import jax
import jax.numpy as jnp

D = 2048
HEADS = 32
HD = 64
TOK_DEV = 768
SPAN = 24576
LEN = 49152
BATCH = 2
N_TP = 2


def draw_cum_gate(key, part):
    keys = jax.random.split(jax.random.fold_in(key, 7), 5)
    fast = jax.random.randint(keys[0], (BATCH, HEADS, 1), 0, 2) == 1
    spread = jnp.exp(jax.random.uniform(keys[1], (BATCH, HEADS, 1), jnp.float32, -0.7, 0.7))
    rate = jnp.where(fast, spread / 40.0, spread / LEN)
    blocks = LEN // TOK_DEV
    factor = jnp.exp(jax.random.uniform(keys[2], (BATCH, HEADS, blocks, 1), jnp.float32, -0.85, 0.85))
    factor = jnp.broadcast_to(factor, (BATCH, HEADS, blocks, TOK_DEV)).reshape(BATCH, HEADS, LEN)
    rough = jax.random.uniform(keys[3], (BATCH, HEADS, LEN), jnp.float32, 0.5, 1.5)
    log_gate = -rate * factor * rough
    start = -jax.random.uniform(keys[4], (BATCH, HEADS, 1), jnp.float32, 0.0, 300.0)
    total = start + jnp.cumsum(log_gate, axis=-1)
    return total.reshape(BATCH, HEADS, N_TP, SPAN).astype(jnp.float32)


def steps_of(key, shape, cuts, smallest, largest):
    factor_of, own = 1.0, jax.random.fold_in(key, 6)
    for axis_at, blocks in cuts:
        steps = jnp.exp(jax.random.uniform(jax.random.fold_in(own, axis_at), (blocks,), jnp.float32, smallest / len(cuts), largest / len(cuts)))
        factor_of = factor_of * jnp.repeat(steps, shape[axis_at] // blocks).reshape([-1 if axis == axis_at else 1 for axis in range(len(shape))])
    return factor_of


def normal_values(key, shape, scale, most, pieces=(), held_as=jnp.bfloat16):
    values = jax.random.normal(key, shape, jnp.float32) * scale
    if len(pieces) > 0:
        values = steps_of(key, shape, pieces, -0.22, 0.18) * values
    return jnp.clip(values, min=-most, max=most).astype(held_as)


def setup_inputs(seed: int = 0) -> dict:
    key_of = jax.random.split(jax.random.key(seed), 6)
    tokens = normal_values(key_of[0], (BATCH, N_TP, SPAN, D), 1.0, 6.0, ((0, 2), (1, 2), (2, 32)))
    key_weight = normal_values(key_of[1], (D, HEADS * HD), D ** -0.5, 0.125)
    value_weight = normal_values(key_of[2], (D, HEADS * HD), D ** -0.5, 0.125)
    cum_gate = draw_cum_gate(jax.random.fold_in(key_of[5], 71), 0)
    query = normal_values(key_of[4], (BATCH, HEADS, HD), 3.0, 12.0, ((0, 2), (1, 32)))
    return dict(tokens=tokens, key_weight=key_weight, value_weight=value_weight, cum_gate=cum_gate, query=query)


def reference(tokens, key_weight, value_weight, cum_gate, query):
    count = tokens.shape[0]
    rows = tokens.reshape(count * LEN, D)

    def project(weight):
        out = jnp.dot(rows, weight, preferred_element_type=jnp.float32).astype(jnp.bfloat16)
        return jnp.transpose(out.reshape(count, LEN, HEADS, HD), (0, 2, 1, 3))

    keys = project(key_weight)
    values = project(value_weight)
    kv_cache = jnp.concatenate([keys, values], axis=-1)
    gate_cache = cum_gate.reshape(count, HEADS, LEN)
    scores = jnp.einsum("bhe,bhse->bhs", query.astype(jnp.float32), keys.astype(jnp.float32))
    scores = scores * (HD ** -0.5) - gate_cache
    top = jnp.max(scores, axis=-1, keepdims=True)
    weights = jnp.exp(scores - top)
    total = jnp.sum(weights, axis=-1)
    probs = weights.astype(jnp.bfloat16).astype(jnp.float32)
    weighted = jnp.einsum("bhs,bhse->bhe", probs, values.astype(jnp.float32))
    read = (weighted / total[..., None]).astype(jnp.bfloat16)
    return kv_cache, gate_cache, read
```

```python
import functools

import jax
import jax.numpy as jnp
from jax import lax
from jax.experimental import pallas as pl
from jax.experimental.pallas import tpu as pltpu
from jax.sharding import PartitionSpec as P

MESH = pl.DeviceIdType.MESH
NX, NY, NZ = 4, 4, 2
COLORS = 3
GROUPS = NY * NZ
NEAR = (1, 3, 2)
F32 = jnp.float32
BF16 = jnp.bfloat16


def group_step(g):
    h, r = g // 4, g % 4
    dy = (1 - h) * (1 + 2 * (r % 2)) + h * (2 - 2 * (r // 2))
    dz = (1 - h) * (1 - r // 2) + h * (1 - r % 2)
    return dy, dz


G_OF = {group_step(g): g for g in range(GROUPS)}


def exchange_kernel(
    tok_hbm, kw_hbm, vw_hbm, gate_hbm, q_ref,
    kv_ref, gate_ref, read_ref,
    tok, w, sr0, sr1, sr2, t0, t1, t2, gin, gr, gt, q8, m_ref, l_ref, a_ref, stat, peer,
    tok_sem, w_sem, gl_sem,
    s10, r10, s11, r11, s12, r12,
    s20, r20, s21, r21, s22, r22,
    s30, r30, s31, r31, s32, r32,
    sg1, rg1, sg2, rg2, sg3, rg3, st, rt,
):
    grp, sp, tp = (lax.axis_index(n) for n in ("gr", "sp", "tp"))
    x, y, z = sp % NX, (sp // NX) % NY, sp // (NX * NY)
    oz = 1 - z
    rows = tok.shape[0]
    unit = rows // COLORS
    half = q_ref.shape[-1]
    cols = w.shape[-1]
    scale = half ** (-0.5)

    def dev(xx, yy, zz):
        return (grp, zz * (NX * NY) + yy * NX + xx, tp)

    def px(d):
        return (x + d) % NX

    def py(d):
        return (y + d) % NY

    def send(src, dst, ssem, rsem, to):
        pltpu.make_async_remote_copy(
            src_ref=src, dst_ref=dst, send_sem=ssem, recv_sem=rsem, device_id=to, device_id_type=MESH
        ).start()

    def done(ref, sem):
        pltpu.make_async_copy(ref, ref, sem).wait()

    def weight_loads(g):
        dy, dz = group_step(g)
        at = (((z + dz) % NZ) * NY + py(dy)) * cols
        at = pl.multiple_of(at, cols)
        return (
            pltpu.make_async_copy(kw_hbm.at[:, pl.ds(at, cols)], w.at[g, 0], w_sem.at[g, 0]),
            pltpu.make_async_copy(vw_hbm.at[:, pl.ds(at, cols)], w.at[g, 1], w_sem.at[g, 1]),
        )

    tok_load = pltpu.make_async_copy(tok_hbm, tok, tok_sem)
    tok_load.start()
    for load in weight_loads(0):
        load.start()
    gate_loads = (
        pltpu.make_async_copy(gate_hbm, gin, gl_sem.at[0]),
        pltpu.make_async_copy(gate_hbm.at[:, :, x], gr.at[x], gl_sem.at[1]),
    )
    for load in gate_loads:
        load.start()
    for load in weight_loads(1):
        load.start()

    barrier = pltpu.get_barrier_semaphore()
    peers = [dev(px(d), y, z) for d in NEAR] + [dev(x, py(d), z) for d in NEAR]
    peers += [dev(x, y, oz), (grp, sp, 1 - tp)]
    for p in peers:
        pl.semaphore_signal(barrier, inc=1, device_id=p, device_id_type=MESH)

    query = jnp.concatenate([q_ref[...].astype(F32), jnp.zeros((1, half), F32)], axis=-1)
    q8[...] = jnp.broadcast_to(query, q8.shape).astype(BF16)
    m_ref[...] = jnp.full(m_ref.shape, -1e30, F32)
    l_ref[...] = jnp.zeros(l_ref.shape, F32)
    a_ref[...] = jnp.zeros(a_ref.shape, F32)

    lane = lax.broadcasted_iota(jnp.int32, (unit, 2 * half), 1)

    def compute(g):
        dy, dz = group_step(g)
        yb, zb = py(dy), (z + dz) % NZ
        slot1 = yb + NY * (1 - (dy + 3) // 4)
        slot2 = zb + NZ * (1 - dz)
        for load in weight_loads(g):
            load.wait()
        for c in range(COLORS):
            left = tok[c * unit : (c + 1) * unit, :]
            k = jnp.dot(left, w[g, 0], preferred_element_type=F32)
            v = jnp.dot(left, w[g, 1], preferred_element_type=F32)
            for j in range(NX):
                at = (j // 2) * 2 * half
                kk, vv = k[:, at : at + 2 * half], v[:, at : at + 2 * half]
                if j % 2 == 0:
                    both = jnp.where(lane < half, kk, pltpu.roll(vv, half, 1))
                else:
                    both = jnp.where(lane < half, pltpu.roll(kk, half, 1), vv)
                both = both.astype(BF16)
                if c == 0:
                    slot0 = j + NX * (1 - ((j + NX - x) % NX + NX - 1) // NX)
                    sr0[slot0, yb, zb] = both
                elif c == 1:
                    sr1[slot1, zb, j] = both
                else:
                    sr2[slot2, j, yb] = both

    def first_sends(g):
        dy, dz = group_step(g)
        yb, zb = py(dy), (z + dz) % NZ

        def along_y():
            send(sr1.at[yb, zb], sr1.at[NY + y, zb], s11.at[g], r11.at[g], dev(x, yb, z))

        def along_z():
            send(sr2.at[zb, :, yb], sr2.at[NZ + z, :, yb], s12.at[g], r12.at[g], dev(x, y, oz))

        if isinstance(g, int):
            if dy != 0:
                along_y()
            if dz != 0:
                along_z()
        else:
            pl.when(dy != 0)(along_y)
            pl.when(dz != 0)(along_z)
        for d in NEAR:
            send(sr0.at[px(d), yb, zb], sr0.at[NX + x, yb, zb], s10.at[g, d], r10.at[g, d], dev(px(d), y, z))

    tok_load.wait()
    compute(0)
    for load in weight_loads(2):
        load.start()
    pl.semaphore_wait(barrier, len(peers))
    first_sends(0)
    for load in gate_loads:
        load.wait()
    for d in NEAR:
        send(gin.at[:, :, px(d)], gr.at[x], sg1.at[d], rg1.at[d], dev(px(d), y, z))

    def step(g, carry):
        @pl.when(g < GROUPS - 2)
        def _():
            for load in weight_loads(g + 2):
                load.start()

        compute(g)
        first_sends(g)
        return carry

    lax.fori_loop(1, GROUPS, step, 0)

    def fwd0(dy, dx):
        sx = (x + NX - dx) % NX
        send(sr0.at[NX + sx, py(dy)], t0.at[y, sx], s20.at[dy, dx], r20.at[dy, dx], dev(x, py(dy), z))

    def fwd1(dy):
        sy = (y + NY - dy) % NY
        send(sr1.at[NY + sy, oz], t1.at[z, sy], s21.at[dy], r21.at[dy], dev(x, y, oz))

    def fwd2(dx, dz):
        sz = (z + dz) % NZ
        send(sr2.at[NZ + sz, px(dx)], t2.at[x, sz], s22.at[dx, dz], r22.at[dx, dz], dev(px(dx), y, z))

    def got10(dy, dz, dx):
        g = G_OF[(dy, dz)]
        done(sr0.at[NX + (x + NX - dx) % NX, py(dy), (z + dz) % NZ], r10.at[g, dx])

    def got11(dy, dz):
        g = G_OF[(dy, dz)]
        done(sr1.at[NY + (y + NY - dy) % NY, (z + dz) % NZ], r11.at[g])

    def got12(dy):
        g = G_OF[(dy, 1)]
        done(sr2.at[NZ + oz, :, py(dy)], r12.at[g])

    fwd1(0)
    for d in NEAR:
        fwd0(d, 0)
        fwd2(d, 0)
    for d in NEAR:
        done(gr.at[(x + NX - d) % NX], rg1.at[d])
    gt[y] = gr[:, :, y]
    got11(1, 1)
    fwd1(1)
    got11(3, 1)
    fwd1(3)
    for dx in NEAR:
        for dy in NEAR[:2]:
            got10(dy, 1, dx)
            got10(dy, 0, dx)
            fwd0(dy, dx)
    for d in NEAR:
        send(gr.at[:, :, py(d)], gt.at[y], sg2.at[d], rg2.at[d], dev(x, py(d), z))
    got11(2, 1)
    fwd1(2)
    for dx in NEAR:
        got10(2, 1, dx)
        got10(2, 0, dx)
        fwd0(2, dx)
    for dy in (1, 3, 2, 0):
        got12(dy)
    for dx in NEAR:
        fwd2(dx, 1)

    def out0(dy):
        sy = (y + NY - dy) % NY
        src = sr0.at[pl.ds(NX, NX), y, oz] if dy == 0 else t0.at[sy, :, oz]
        send(src, kv_ref.at[z, sy, :, 0], s30.at[dy], r30.at[dy], dev(x, y, oz))

    def out1(dz, dx):
        sz = (z + dz) % NZ
        src = sr1.at[pl.ds(NY, NY), z, px(dx)] if dz == 0 else t1.at[sz, :, px(dx)]
        send(src, kv_ref.at[sz, :, x, 1], s31.at[dz, dx], r31.at[dz, dx], dev(px(dx), y, z))

    def out2(dx, dy):
        sx = (x + NX - dx) % NX
        src = sr2.at[pl.ds(NZ, NZ), x, py(dy)] if dx == 0 else t2.at[sx, :, py(dy)]
        send(src, kv_ref.at[:, y, sx, 2], s32.at[dx, dy], r32.at[dx, dy], dev(x, py(dy), z))

    for dx in NEAR:
        got10(0, 1, dx)
    out0(0)
    for dy in NEAR:
        got11(dy, 0)
    for d in NEAR:
        out1(0, d)
        out2(0, d)
    for dx in NEAR:
        got10(0, 0, dx)

    def attend(kv, gate):
        s = lax.dot_general(q8[...], kv, (((1,), (1,)), ((), ())), preferred_element_type=F32)
        s = s * scale - gate
        old = m_ref[...]
        top = jnp.maximum(old, jnp.max(s, axis=1, keepdims=True))
        p = jnp.exp(s - top[:, :1])
        keep = jnp.exp(old - top)
        m_ref[...] = top
        l_ref[...] = l_ref[...] * keep + jnp.sum(p, axis=1, keepdims=True)
        a_ref[...] = a_ref[...] * keep + jnp.dot(p.astype(BF16), kv, preferred_element_type=F32)

    def attend0(sz, sy):
        kv = kv_ref[sz, sy, :, 0].reshape(NX * unit, 2 * half)
        gate = jnp.concatenate([gate_ref[sz, sy, k, :, 0:unit] for k in range(NX)], axis=-1)
        attend(kv, gate)

    def attend1(sz, sx):
        kv = kv_ref[sz, :, sx, 1].reshape(NY * unit, 2 * half)
        gate = jnp.concatenate([gate_ref[sz, k, sx, :, unit : 2 * unit] for k in range(NY)], axis=-1)
        attend(kv, gate)

    def attend2(sy, sx):
        kv = kv_ref[:, sy, sx, 2].reshape(NZ * unit, 2 * half)
        gate = jnp.concatenate([gate_ref[k, sy, sx, :, 2 * unit : 3 * unit] for k in range(NZ)], axis=-1)
        attend(kv, gate)

    def keep0(dy):
        sy = (y + NY - dy) % NY
        kv_ref[z, sy, :, 0] = sr0[NX : 2 * NX, y, z] if dy == 0 else t0[sy, :, z]

    def keep1(dz):
        sz = (z + dz) % NZ
        kv_ref[sz, :, x, 1] = sr1[NY : 2 * NY, z, x] if dz == 0 else t1[sz, :, x]

    def keep2(dx):
        sx = (x + NX - dx) % NX
        kv_ref[:, y, sx, 2] = sr2[NZ : 2 * NZ, x, y] if dx == 0 else t2[sx, :, y]

    for d in NEAR:
        done(gt.at[(y + NY - d) % NY], rg2.at[d])
    send(gt.at[:, :, oz], gate_ref.at[z], sg3.at[0], rg3.at[0], dev(x, y, oz))
    gate_ref[z] = gt[:, :, z]
    keep0(0)
    keep1(0)
    keep2(0)

    def got20(dy):
        sy = (y + NY - dy) % NY
        for dx in (0, 1, 3, 2):
            done(t0.at[sy, (x + NX - dx) % NX], r20.at[dy, dx])

    def got22(dx):
        for dz in range(NZ):
            done(t2.at[(x + NX - dx) % NX, (z + dz) % NZ], r22.at[dx, dz])

    for dy in NEAR[:2]:
        got20(dy)
        out0(dy)
    got20(2)
    out0(2)
    for dx in NEAR[:2]:
        got22(dx)
        for d in NEAR:
            out2(dx, d)
    for dy in range(NY):
        done(t1.at[oz, (y + NY - dy) % NY], r21.at[dy])
    for d in NEAR:
        out1(1, d)
    got22(2)
    for d in NEAR:
        out2(2, d)
    for d in NEAR:
        keep0(d)
        keep2(d)
    keep1(1)
    done(gate_ref.at[oz], rg3.at[0])

    def local_attend(i, carry):
        attend0(z, i)
        attend2(y, i)
        return carry

    lax.fori_loop(0, NX, local_attend, 0)
    attend1(0, x)
    attend1(1, x)

    def arrive0(dy):
        sy = (y + NY - dy) % NY
        done(kv_ref.at[oz, sy, :, 0], r30.at[dy])
        attend0(oz, sy)

    def arrive1(dz, dx):
        sz, sx = (z + dz) % NZ, (x + NX - dx) % NX
        done(kv_ref.at[sz, :, sx, 1], r31.at[dz, dx])
        attend1(sz, sx)

    def arrive2(dx, dy):
        sx, sy = (x + NX - dx) % NX, (y + NY - dy) % NY
        done(kv_ref.at[:, sy, sx, 2], r32.at[dx, dy])
        attend2(sy, sx)

    arrive0(0)
    for d in NEAR:
        arrive1(0, d)
        arrive2(0, d)
    arrive0(1)
    arrive0(3)
    for dx in NEAR[:2]:
        for d in NEAR:
            arrive2(dx, d)
    arrive0(2)
    for d in NEAR:
        arrive1(1, d)
        arrive2(2, d)

    stat[0:1, :] = m_ref[0:1, :]
    stat[1:2, :] = l_ref[0:1, :]
    stat[2:3, :] = a_ref[0:1, :]
    swap = pltpu.make_async_remote_copy(
        src_ref=stat, dst_ref=peer, send_sem=st.at[0], recv_sem=rt.at[0],
        device_id=(grp, sp, 1 - tp), device_id_type=MESH,
    )
    swap.start()

    for g in range(GROUPS):
        dy, dz = group_step(g)
        yb, zb = py(dy), (z + dz) % NZ
        for d in NEAR:
            done(sr0.at[px(d), yb, zb], s10.at[g, d])
        if dy != 0:
            done(sr1.at[yb, zb], s11.at[g])
        if dz != 0:
            done(sr2.at[zb, :, yb], s12.at[g])
    for d in NEAR:
        for k in range(NX):
            done(t0.at[y, k], s20.at[d, k])
        for k in range(NZ):
            done(t2.at[x, k], s22.at[d, k])
        done(gr.at[x], sg1.at[d])
        done(gt.at[y], sg2.at[d])
        for k in range(NZ):
            done(kv_ref.at[0, :, x, 1], s31.at[k, d])
        for k in range(NX):
            done(kv_ref.at[:, y, 0, 2], s32.at[k, d])
    for k in range(NY):
        done(t1.at[z, k], s21.at[k])
        done(kv_ref.at[z, k, :, 0], s30.at[k])
    done(gate_ref.at[z], sg3.at[0])
    swap.wait()

    mine, theirs = stat[...], peer[...]
    first = jnp.where(tp == 0, mine, theirs)
    second = jnp.where(tp == 0, theirs, mine)
    top = jnp.maximum(first[0:1], second[0:1])
    e1, e2 = jnp.exp(first[0:1] - top), jnp.exp(second[0:1] - top)
    total = first[1:2] * e1 + second[1:2] * e2
    weighted = first[2:3] * e1 + second[2:3] * e2
    read_ref[0] = (weighted / total)[:, half:].astype(BF16)


def store_kernel(kv_ref, gate_ref, read_ref, kv_out, gate_out, read_out, sem):
    copies = []
    for k in range(NZ):
        for j in range(NY):
            copies.append(pltpu.make_async_copy(kv_ref.at[k, j], kv_out.at[k, j], sem.at[len(copies)]))
    copies.append(pltpu.make_async_copy(gate_ref, gate_out, sem.at[len(copies)]))
    copies.append(pltpu.make_async_copy(read_ref, read_out, sem.at[len(copies)]))
    for c in copies:
        c.start()
    for c in copies:
        c.wait()


def on_device(tokens, key_weight, value_weight, cum_gate, query):
    rows, width = tokens.shape[2:]
    hd = query.shape[2]
    unit = rows // COLORS
    cols = NX * hd
    kv_shape = (NZ, NY, NX, COLORS, unit, 2 * hd)
    gate_shape = (NZ, NY, NX, 1, rows)
    read_shape = (1, 1, hd)
    vmem = pl.BlockSpec(memory_space=pltpu.VMEM)
    anywhere = pl.BlockSpec(memory_space=pl.ANY)
    dma = pltpu.SemaphoreType.DMA
    u = (unit, 2 * hd)
    kv, gate, read = pl.pallas_call(
        exchange_kernel,
        out_shape=[pltpu.VMEM(kv_shape, BF16), pltpu.VMEM(gate_shape, F32), pltpu.VMEM(read_shape, BF16)],
        in_specs=[anywhere, anywhere, anywhere, anywhere, vmem],
        out_specs=[vmem, vmem, vmem],
        scratch_shapes=[
            pltpu.VMEM((rows, width), BF16),
            pltpu.VMEM((GROUPS, 2, width, cols), BF16),
            pltpu.VMEM((2 * NX, NY, NZ, *u), BF16),
            pltpu.VMEM((2 * NY, NZ, NX, *u), BF16),
            pltpu.VMEM((2 * NZ, NX, NY, *u), BF16),
            pltpu.VMEM((NY, NX, NZ, *u), BF16),
            pltpu.VMEM((NZ, NY, NX, *u), BF16),
            pltpu.VMEM((NX, NZ, NY, *u), BF16),
            pltpu.VMEM(gate_shape, F32),
            pltpu.VMEM((NX, NZ, NY, 1, rows), F32),
            pltpu.VMEM((NY, NX, NZ, 1, rows), F32),
            pltpu.VMEM((8, 2 * hd), BF16),
            pltpu.VMEM((8, 2 * hd), F32),
            pltpu.VMEM((8, 2 * hd), F32),
            pltpu.VMEM((8, 2 * hd), F32),
            pltpu.VMEM((8, 2 * hd), F32),
            pltpu.VMEM((8, 2 * hd), F32),
            dma(()), dma((GROUPS, 2)), dma((2,)),
            dma((GROUPS, NX)), dma((GROUPS, NX)), dma((GROUPS,)), dma((GROUPS,)), dma((GROUPS,)), dma((GROUPS,)),
            dma((NY, NX)), dma((NY, NX)), dma((NY,)), dma((NY,)), dma((NX, NZ)), dma((NX, NZ)),
            dma((NY,)), dma((NY,)), dma((NZ, NX)), dma((NZ, NX)), dma((NX, NY)), dma((NX, NY)),
            dma((NX,)), dma((NX,)), dma((NY,)), dma((NY,)), dma((1,)), dma((1,)), dma((1,)), dma((1,)),
        ],
        compiler_params=pltpu.CompilerParams(
            collective_id=0, has_side_effects=True, vmem_limit_bytes=50 * 2**20
        ),
        name="exchange",
    )(tokens.reshape(rows, width), key_weight, value_weight, cum_gate.reshape(gate_shape), query.reshape(1, hd))
    kv, gate, read = pl.pallas_call(
        store_kernel,
        out_shape=[
            jax.ShapeDtypeStruct(kv_shape, BF16),
            jax.ShapeDtypeStruct(gate_shape, F32),
            jax.ShapeDtypeStruct(read_shape, BF16),
        ],
        in_specs=[vmem, vmem, vmem],
        out_specs=[anywhere, anywhere, anywhere],
        scratch_shapes=[dma((NZ * NY + 2,))],
        compiler_params=pltpu.CompilerParams(vmem_limit_bytes=2**20),
        name="store",
    )(kv, gate, read)
    length = NX * NY * NZ * rows
    return kv.reshape(1, 1, length, 2 * hd), gate.reshape(1, 1, length), read


def solution(mesh):
    placed = (P("gr", "tp", "sp", None), P(), P(), P("gr", None, "tp", "sp"), P("gr", "sp", None))
    return jax.shard_map(
        on_device,
        mesh=mesh,
        in_specs=placed,
        out_specs=(P("gr", "sp", "tp", None), P("gr", "sp", "tp"), P("gr", "sp", None)),
        check_vma=False,
    )
```

```python
import functools

import jax
import jax.numpy as jnp
from jax import lax
from jax.experimental import pallas as pl
from jax.experimental.pallas import tpu as pltpu
from jax.sharding import PartitionSpec as P

MESH = pl.DeviceIdType.MESH
NX, NY, NZ = 4, 4, 2
COLORS = 3
GROUPS = NY * NZ
NEAR = (1, 3, 2)
F32 = jnp.float32
BF16 = jnp.bfloat16


def group_step(g):
    h, r = g // 4, g % 4
    dy = (1 - h) * (1 + 2 * (r % 2)) + h * (2 - 2 * (r // 2))
    dz = (1 - h) * (1 - r // 2) + h * (1 - r % 2)
    return dy, dz


def exchange_kernel(
    tok_hbm, kw_hbm, vw_hbm, gate_hbm, q_ref,
    kv_ref, gate_ref, stat, peer,
    tok, w, sr0, sr1, sr2, t0, t1, t2, gin, gr, gt, q8, m_ref, l_ref, a_ref,
    tok_sem, w_sem, gl_sem, out_sem, gs_sem, gd_sem,
    r10, r11, r12, r20, r21, r22, r30, r31, r32, st, rt,
):
    grp, sp, tp = (lax.axis_index(n) for n in ("gr", "sp", "tp"))
    x, y, z = sp % NX, (sp // NX) % NY, sp // (NX * NY)
    oz = 1 - z
    unit = tok.shape[0] // COLORS
    half = q_ref.shape[-1]
    pair = 2 * half
    cols = NX * half
    scale = half ** (-0.5)

    def dev(xx, yy, zz):
        return (grp, zz * (NX * NY) + yy * NX + xx, tp)

    def px(d):
        return (x + d) % NX

    def py(d):
        return (y + d) % NY

    def bx(d):
        return (x + NX - d) % NX

    def by(d):
        return (y + NY - d) % NY

    def send(src, dst, ssem, rsem, to):
        pltpu.make_async_remote_copy(
            src_ref=src, dst_ref=dst, send_sem=ssem, recv_sem=rsem, device_id=to, device_id_type=MESH
        ).start()

    def done(ref, sem):
        pltpu.make_async_copy(ref, ref, sem).wait()

    def load_tokens(c):
        at = pl.ds(c * unit, unit)
        pltpu.make_async_copy(tok_hbm.at[at], tok.at[at], tok_sem.at[c]).start()

    def load_weights(g, h, sem):
        dy, dz = group_step(g)
        at = pl.multiple_of((((z + dz) % NZ) * NY + py(dy)) * cols, cols) + h * pair
        left, right = w.at[g, h, :, pl.ds(0, pair)], w.at[g, h, :, pl.ds(pair, pair)]
        pltpu.make_async_copy(kw_hbm.at[:, pl.ds(at, pair)], left, w_sem.at[sem]).start()
        pltpu.make_async_copy(vw_hbm.at[:, pl.ds(at, pair)], right, w_sem.at[sem]).start()

    def load_group(g):
        load_weights(g, 0, g)
        load_weights(g, 1, g)

    def tokens_here(c):
        done(tok.at[pl.ds(c * unit, unit)], tok_sem.at[c])

    load_weights(0, 0, 0)
    load_tokens(1)
    load_weights(1, 0, 1)
    load_tokens(0)
    load_tokens(2)

    barrier = pltpu.get_barrier_semaphore()
    peers = [dev(px(d), y, z) for d in NEAR] + [dev(x, py(d), z) for d in NEAR]
    peers += [dev(x, y, oz), (grp, sp, 1 - tp)]
    for p in peers:
        pl.semaphore_signal(barrier, inc=1, device_id=p, device_id_type=MESH)

    query = jnp.concatenate([q_ref[...].astype(F32), jnp.zeros((1, half), F32)], axis=-1)
    q8[...] = jnp.broadcast_to(query, q8.shape).astype(BF16)
    m_ref[...] = jnp.full(m_ref.shape, -1e30, F32)
    l_ref[...] = jnp.zeros(l_ref.shape, F32)
    a_ref[...] = jnp.zeros(a_ref.shape, F32)

    lane = lax.broadcasted_iota(jnp.int32, (unit, 2 * half), 1)

    def compute(*steps):
        made = []
        for g, h, c in steps:
            left = tok[c * unit : (c + 1) * unit, :]
            made.append(jnp.dot(left, w[g, h], preferred_element_type=F32))
        for (g, h, c), kv in zip(steps, made):
            dy, dz = group_step(g)
            yb, zb = py(dy), (z + dz) % NZ
            k, v = kv[:, :pair], kv[:, pair:]
            first = jnp.where(lane < half, k, pltpu.roll(v, half, 1)).astype(BF16)
            second = jnp.where(lane < half, pltpu.roll(k, half, 1), v).astype(BF16)
            for j, both in ((2 * h, first), (2 * h + 1, second)):
                if c == 0:
                    sr0[j + NX * (1 - ((j + NX - x) % NX + NX - 1) // NX), yb, zb] = both
                elif c == 1:
                    sr1[yb + NY * (1 - (dy + NY - 1) // NY), zb, j] = both
                else:
                    sr2[zb + NZ * (1 - dz), j, yb] = both

    def half_sends(g, h, c):
        dy, dz = group_step(g)
        yb, zb = py(dy), (z + dz) % NZ
        two = pl.ds(2 * h, 2)
        if c == 0:
            for j in (2 * h, 2 * h + 1):

                @pl.when(x != j)
                def _():
                    d = (j + NX - x) % NX
                    send(sr0.at[j, yb, zb], sr0.at[NX + x, yb, zb], out_sem.at[0], r10.at[dy, d - 1], dev(j, y, z))
        elif c == 1:
            send(sr1.at[yb, zb, two], sr1.at[NY + y, zb, two], out_sem.at[1], r11.at[dy - 1, dz], dev(x, yb, z))
        else:
            send(sr2.at[zb, two, yb], sr2.at[NZ + z, two, yb], out_sem.at[2], r12.at[0], dev(x, y, oz))

    def along_x(dy, dz):
        yb = py(dy)
        at = (yb,) if dz is None else (yb, (z + dz) % NZ)
        for d in NEAR:
            send(
                sr0.at[(px(d), *at)], sr0.at[(NX + x, *at)], out_sem.at[0], r10.at[dy, d - 1], dev(px(d), y, z)
            )

    def along_y(g):
        dy, dz = group_step(g)
        yb, zb = py(dy), (z + dz) % NZ
        send(sr1.at[yb, zb], sr1.at[NY + y, zb], out_sem.at[1], r11.at[dy - 1, dz], dev(x, yb, z))

    def along_z(g):
        yb, zb = py(group_step(g)[0]), oz
        send(sr2.at[zb, :, yb], sr2.at[NZ + z, :, yb], out_sem.at[2], r12.at[0], dev(x, y, oz))

    def whole(g, c):
        compute((g, 0, c), (g, 1, c))

    done(w.at[0, 0], w_sem.at[0])
    tokens_here(1)
    done(w.at[1, 0], w_sem.at[1])
    load_weights(0, 1, GROUPS)
    load_weights(1, 1, GROUPS + 1)
    compute((0, 0, 1), (1, 0, 1))
    pl.semaphore_wait(barrier, len(peers))
    half_sends(0, 0, 1)
    half_sends(1, 0, 1)
    tokens_here(0)
    tokens_here(2)
    load_group(3)
    load_group(2)
    gate_loads = (
        pltpu.make_async_copy(gate_hbm, gin, gl_sem.at[0]),
        pltpu.make_async_copy(gate_hbm.at[:, :, x], gr.at[x], gl_sem.at[1]),
    )
    for load in gate_loads:
        load.start()
    compute((0, 0, 0), (0, 0, 2))
    half_sends(0, 0, 2)
    half_sends(0, 0, 0)
    done(w.at[0, 1], w_sem.at[GROUPS])
    compute((0, 1, 0), (0, 1, 2))
    half_sends(0, 1, 2)
    half_sends(0, 1, 0)
    load_group(4)
    load_group(5)
    done(w.at[1, 1], w_sem.at[GROUPS + 1])
    compute((0, 1, 1), (1, 1, 1))
    half_sends(0, 1, 1)
    half_sends(1, 1, 1)
    for load in gate_loads:
        load.wait()
    for d in NEAR:
        send(gin.at[:, :, px(d)], gr.at[x], gs_sem.at[0], gd_sem.at[0], dev(px(d), y, z))
    whole(1, 0)
    done(w.at[3], w_sem.at[3])
    whole(3, 0)
    along_x(3, None)
    load_group(6)
    load_group(7)
    done(w.at[2], w_sem.at[2])
    whole(2, 1)
    along_y(2)
    whole(3, 1)
    along_y(3)
    whole(1, 2)
    along_z(1)
    whole(2, 0)
    along_x(1, 0)
    done(w.at[4], w_sem.at[4])
    whole(4, 1)
    along_y(4)
    whole(4, 2)
    along_z(4)
    whole(4, 0)
    done(w.at[5], w_sem.at[5])
    whole(5, 0)
    along_x(2, None)
    done(gr.at[0 : NX - 1], gd_sem.at[0])
    gt[y] = gr[:, :, y]
    for d in NEAR:
        send(gr.at[:, :, py(d)], gt.at[y], gs_sem.at[1], gd_sem.at[1], dev(x, py(d), z))
    whole(5, 1)
    along_y(5)
    done(w.at[6], w_sem.at[6])
    whole(6, 2)
    along_z(6)
    whole(6, 0)
    done(w.at[7], w_sem.at[7])
    whole(7, 0)
    along_x(0, None)
    for g, c in ((6, 1), (7, 1), (2, 2), (3, 2), (5, 2), (7, 2)):
        whole(g, c)

    def fwd0(dy, dx):
        send(sr0.at[NX + bx(dx), py(dy)], t0.at[y, bx(dx)], out_sem.at[0], r20.at[dy - 1], dev(x, py(dy), z))

    def fwd1(dy):
        send(sr1.at[NY + by(dy), oz], t1.at[z, by(dy)], out_sem.at[1], r21.at[0], dev(x, y, oz))

    def fwd2(dx, dz):
        sz = (z + dz) % NZ
        send(sr2.at[NZ + sz, px(dx)], t2.at[x, sz], out_sem.at[2], r22.at[dx - 1], dev(px(dx), y, z))

    def got10(dy, dx):
        done(sr0.at[NX + bx(dx), py(dy)], r10.at[dy, dx - 1])

    def got11(dy, dz):
        done(sr1.at[NY + by(dy), (z + dz) % NZ], r11.at[dy - 1, dz])

    def got20(dy):
        done(t0.at[by(dy)], r20.at[dy - 1])

    def got22(dx):
        done(t2.at[bx(dx)], r22.at[dx - 1])

    def out0(dy):
        src = sr0.at[pl.ds(NX, NX), y, oz] if dy == 0 else t0.at[by(dy), :, oz]
        send(src, kv_ref.at[z, by(dy), :, 0], out_sem.at[0], r30.at[dy], dev(x, y, oz))

    def out1(dz, dx):
        sz = (z + dz) % NZ
        src = sr1.at[pl.ds(NY, NY), z, px(dx)] if dz == 0 else t1.at[sz, :, px(dx)]
        send(src, kv_ref.at[sz, :, x, 1], out_sem.at[1], r31.at[dz, dx - 1], dev(px(dx), y, z))

    def out2(dx, dy):
        src = sr2.at[pl.ds(NZ, NZ), x, py(dy)] if dx == 0 else t2.at[bx(dx), :, py(dy)]
        send(src, kv_ref.at[:, y, bx(dx), 2], out_sem.at[2], r32.at[dx, dy - 1], dev(x, py(dy), z))

    def keep0(dy):
        kv_ref[z, by(dy), :, 0] = sr0[NX : 2 * NX, y, z] if dy == 0 else t0[by(dy), :, z]

    def keep1(dz):
        sz = (z + dz) % NZ
        kv_ref[sz, :, x, 1] = sr1[NY : 2 * NY, z, x] if dz == 0 else t1[sz, :, x]

    def keep2(dx):
        kv_ref[:, y, bx(dx), 2] = sr2[NZ : 2 * NZ, x, y] if dx == 0 else t2[bx(dx), :, y]

    def come0(dy):
        done(kv_ref.at[oz, by(dy), :, 0], r30.at[dy])

    def come1(dz, dx):
        done(kv_ref.at[(z + dz) % NZ, :, bx(dx), 1], r31.at[dz, dx - 1])

    def come2(dx, dy):
        done(kv_ref.at[:, by(dy), bx(dx), 2], r32.at[dx, dy - 1])

    def part0(sz, sy):
        gates = [gate_ref[sz, sy, k, :, 0:unit] for k in range(NX)]
        return kv_ref[sz, sy, :, 0].reshape(NX * unit, 2 * half), gates

    def part1(sz, sx):
        gates = [gate_ref[sz, k, sx, :, unit : 2 * unit] for k in range(NY)]
        return kv_ref[sz, :, sx, 1].reshape(NY * unit, 2 * half), gates

    def part2(sy, sx):
        gates = [gate_ref[k, sy, sx, :, 2 * unit : 3 * unit] for k in range(NZ)]
        return kv_ref[:, sy, sx, 2].reshape(NZ * unit, 2 * half), gates

    def folded(op, values):
        width = 2 * half
        pieces = [v[:, i : i + width] for v in values for i in range(0, v.shape[1], width)]
        while len(pieces) > 1:
            pieces = [op(*pieces[i : i + 2]) if i + 1 < len(pieces) else pieces[i] for i in range(0, len(pieces), 2)]
        return pieces[0]

    def attend(parts):
        scores = []
        for kv, gates in parts:
            s = lax.dot_general(q8[...], kv, (((1,), (1,)), ((), ())), preferred_element_type=F32)
            scores.append(s * scale - jnp.concatenate(gates, axis=-1))
        old = m_ref[...]
        top = jnp.maximum(old, jnp.max(folded(jnp.maximum, scores), axis=1, keepdims=True))
        weights = [jnp.exp(s - top[:, :1]) for s in scores]
        keep = jnp.exp(old - top)
        m_ref[...] = top
        l_ref[...] = l_ref[...] * keep + jnp.sum(folded(jnp.add, weights), axis=1, keepdims=True)
        acc = a_ref[...] * keep
        for p, (kv, _) in zip(weights, parts):
            acc = acc + jnp.dot(p.astype(BF16), kv, preferred_element_type=F32)
        a_ref[...] = acc

    fwd1(0)
    for d in NEAR:
        if d != 2:
            fwd0(d, 0)
        fwd2(d, 0)
    done(gt.at[0 : NY - 1], gd_sem.at[1])
    send(gt.at[:, :, oz], gate_ref.at[z], gs_sem.at[2], gd_sem.at[2], dev(x, y, oz))
    gate_ref[z] = gt[:, :, z]
    for dy in NEAR[:2]:
        got11(dy, 1)
        fwd1(dy)
    for dx in NEAR:
        for dy in NEAR[:2]:
            got10(dy, dx)
            fwd0(dy, dx)
    got11(2, 1)
    fwd1(2)
    for dx in NEAR:
        got10(2, dx)
    send(sr0.at[pl.ds(NX, NX), py(2)], t0.at[y], out_sem.at[0], r20.at[1], dev(x, py(2), z))
    done(sr2.at[NZ + oz], r12.at[0])
    for dx in NEAR:
        fwd2(dx, 1)
    for dx in NEAR:
        got10(0, dx)
    out0(0)
    for dy in NEAR:
        got11(dy, 0)
    for d in NEAR:
        out1(0, d)
        out2(0, d)
    keep0(0)
    keep1(0)
    keep2(0)
    done(gate_ref.at[oz], gd_sem.at[2])
    attend([part0(z, y), part1(z, x), part2(y, x)])

    for dy in NEAR[:2]:
        got20(dy)
        out0(dy)
    for dy in NEAR[:2]:
        keep0(dy)
    attend([part0(z, by(1)), part0(z, by(3))])
    for dx in NEAR[:2]:
        got22(dx)
        for d in NEAR:
            out2(dx, d)
    got20(2)
    out0(2)
    done(t1.at[oz], r21.at[0])
    for d in NEAR:
        out1(1, d)
    got22(2)
    for d in NEAR:
        out2(2, d)
    keep0(2)
    keep1(1)
    for d in NEAR:
        keep2(d)
    attend([part0(z, by(2)), part1(oz, x)] + [part2(y, bx(d)) for d in NEAR])

    come0(0)
    come1(0, 1)
    come1(0, 3)
    for d in NEAR:
        come2(0, d)
    attend([part0(oz, y), part1(z, bx(1)), part1(z, bx(3))] + [part2(by(d), x) for d in NEAR])
    come0(1)
    come1(0, 2)
    for d in NEAR:
        come2(1, d)
    attend([part0(oz, by(1)), part1(z, bx(2))] + [part2(by(d), bx(1)) for d in NEAR])
    come0(3)
    come1(1, 1)
    come1(1, 3)
    for d in NEAR:
        come2(3, d)
    attend([part0(oz, by(3)), part1(oz, bx(1)), part1(oz, bx(3))] + [part2(by(d), bx(3)) for d in NEAR])
    come2(2, 1)
    come2(2, 3)
    attend([part2(by(1), bx(2)), part2(by(3), bx(2))])
    come0(2)
    come1(1, 2)
    come2(2, 2)
    attend([part0(oz, by(2)), part1(oz, bx(2)), part2(by(2), bx(2))])

    stat[0:1, :] = m_ref[0:1, :]
    stat[1:2, :] = l_ref[0:1, :]
    stat[2:3, :] = a_ref[0:1, :]
    swap = pltpu.make_async_remote_copy(
        src_ref=stat, dst_ref=peer, send_sem=st.at[0], recv_sem=rt.at[0],
        device_id=(grp, sp, 1 - tp), device_id_type=MESH,
    )
    swap.start()
    done(sr0, out_sem.at[0])
    done(sr1, out_sem.at[1])
    done(sr2, out_sem.at[2])
    done(gr.at[0 : NX - 1], gs_sem.at[0])
    done(gt.at[0 : NY - 1], gs_sem.at[1])
    done(gate_ref.at[z], gs_sem.at[2])
    swap.wait()


def store_kernel(kv_ref, gate_ref, stat, peer, kv_out, gate_out, read_out, read_ref, sem):
    copies = [
        pltpu.make_async_copy(kv_ref.at[k, j], kv_out.at[k, j], sem.at[0]) for k in range(NZ) for j in range(NY)
    ]
    copies.append(pltpu.make_async_copy(gate_ref, gate_out, sem.at[1]))
    for c in copies:
        c.start()
    half = read_ref.shape[-1]
    tp = lax.axis_index("tp")
    first = jnp.where(tp == 0, stat[...], peer[...])
    second = jnp.where(tp == 0, peer[...], stat[...])
    top = jnp.maximum(first[0:1], second[0:1])
    e1, e2 = jnp.exp(first[0:1] - top), jnp.exp(second[0:1] - top)
    total = first[1:2] * e1 + second[1:2] * e2
    weighted = first[2:3] * e1 + second[2:3] * e2
    read_ref[0] = (weighted / total)[:, half:].astype(BF16)
    last = pltpu.make_async_copy(read_ref, read_out, sem.at[2])
    last.start()
    pltpu.make_async_copy(kv_ref, kv_out, sem.at[0]).wait()
    copies[-1].wait()
    last.wait()


def on_device(tokens, key_weight, value_weight, cum_gate, query):
    rows, width = tokens.shape[2:]
    hd = query.shape[2]
    unit = rows // COLORS
    cols = NX * hd
    kv_shape = (NZ, NY, NX, COLORS, unit, 2 * hd)
    gate_shape = (NZ, NY, NX, 1, rows)
    read_shape = (1, 1, hd)
    vmem = pl.BlockSpec(memory_space=pltpu.VMEM)
    anywhere = pl.BlockSpec(memory_space=pl.ANY)
    dma = pltpu.SemaphoreType.DMA
    u = (unit, 2 * hd)
    stat_shape = (8, 2 * hd)
    kv, gate, stat, peer = pl.pallas_call(
        exchange_kernel,
        out_shape=[
            pltpu.VMEM(kv_shape, BF16),
            pltpu.VMEM(gate_shape, F32),
            pltpu.VMEM(stat_shape, F32),
            pltpu.VMEM(stat_shape, F32),
        ],
        in_specs=[anywhere, anywhere, anywhere, anywhere, vmem],
        out_specs=[vmem, vmem, vmem, vmem],
        scratch_shapes=[
            pltpu.VMEM((rows, width), BF16),
            pltpu.VMEM((GROUPS, 2, width, cols), BF16),
            pltpu.VMEM((2 * NX, NY, NZ, *u), BF16),
            pltpu.VMEM((2 * NY, NZ, NX, *u), BF16),
            pltpu.VMEM((2 * NZ, NX, NY, *u), BF16),
            pltpu.VMEM((NY, NX, NZ, *u), BF16),
            pltpu.VMEM((NZ, NY, NX, *u), BF16),
            pltpu.VMEM((NX, NZ, NY, *u), BF16),
            pltpu.VMEM(gate_shape, F32),
            pltpu.VMEM((NX, NZ, NY, 1, rows), F32),
            pltpu.VMEM((NY, NX, NZ, 1, rows), F32),
            pltpu.VMEM((8, 2 * hd), BF16),
            pltpu.VMEM(stat_shape, F32),
            pltpu.VMEM(stat_shape, F32),
            pltpu.VMEM(stat_shape, F32),
            dma((COLORS,)), dma((GROUPS + 2,)), dma((2,)), dma((COLORS,)), dma((3,)), dma((3,)),
            dma((NY, NX - 1)), dma((NY - 1, NZ)), dma((1,)),
            dma((NY - 1,)), dma((1,)), dma((NX - 1,)),
            dma((NY,)), dma((NZ, NX - 1)), dma((NX, NY - 1)), dma((1,)), dma((1,)),
        ],
        compiler_params=pltpu.CompilerParams(
            collective_id=0, has_side_effects=True, vmem_limit_bytes=50 * 2**20
        ),
        name="exchange",
    )(tokens.reshape(rows, width), key_weight, value_weight, cum_gate.reshape(gate_shape), query.reshape(1, hd))
    kv, gate, read = pl.pallas_call(
        store_kernel,
        out_shape=[
            jax.ShapeDtypeStruct(kv_shape, BF16),
            jax.ShapeDtypeStruct(gate_shape, F32),
            jax.ShapeDtypeStruct(read_shape, BF16),
        ],
        in_specs=[vmem] * 4,
        out_specs=[anywhere, anywhere, anywhere],
        scratch_shapes=[pltpu.VMEM(read_shape, BF16), dma((3,))],
        compiler_params=pltpu.CompilerParams(vmem_limit_bytes=2**20),
        name="store",
    )(kv, gate, stat, peer)
    length = NX * NY * NZ * rows
    return kv.reshape(1, 1, length, 2 * hd), gate.reshape(1, 1, length), read


def solution(mesh):
    placed = (P("gr", "tp", "sp", None), P(), P(), P("gr", None, "tp", "sp"), P("gr", "sp", None))
    return jax.shard_map(
        on_device,
        mesh=mesh,
        in_specs=placed,
        out_specs=(P("gr", "sp", "tp", None), P("gr", "sp", "tp"), P("gr", "sp", None)),
        check_vma=False,
    )
```

```python
import functools

import jax
import jax.numpy as jnp
from jax import lax
from jax.experimental import pallas as pl
from jax.experimental.pallas import tpu as pltpu
from jax.sharding import PartitionSpec as P

MESH = pl.DeviceIdType.MESH
NX, NY, NZ = 4, 4, 2
COLORS = 3
GROUPS = NY * NZ
NEAR = (1, 3, 2)
WAY_X1 = (3, 1, 1, 3)
WAY_Y1 = (3, 1)
WAY_X = (1, 3)
WAY_Y = (1, 1, 3, 3)
F32 = jnp.float32
BF16 = jnp.bfloat16


def group_step(g):
    h, r = g // 4, g % 4
    dy = (1 - h) * (1 + 2 * (r % 2)) + h * (2 - 2 * (r // 2))
    dz = (1 - h) * (1 - r // 2) + h * (1 - r % 2)
    return dy, dz


def exchange_kernel(
    tok_hbm, kw_hbm, vw_hbm, gate_hbm, q_ref,
    kv_ref, gate_ref, stat, peer,
    tok, w, sr0, sr1, sr2, t0, t1, t2, qx1, qy1, qx2, qy2, qx3, qy3,
    gin, gr, gt, q8, m_ref, l_ref, a_ref,
    tok_sem, w_sem, gl_sem, out_sem, hop_sem, gs_sem, gd_sem,
    hx1, hy1, hx2, hy2, hx3, hy3,
    r10, r11, r12, r20, r21, r22, r30, r31, r32, st, rt,
):
    grp, sp, tp = (lax.axis_index(n) for n in ("gr", "sp", "tp"))
    x, y, z = sp % NX, (sp // NX) % NY, sp // (NX * NY)
    oz = 1 - z
    unit = tok.shape[0] // COLORS
    half = q_ref.shape[-1]
    pair = 2 * half
    cols = NX * half
    scale = half ** (-0.5)

    def dev(xx, yy, zz):
        return (grp, zz * (NX * NY) + yy * NX + xx, tp)

    def px(d):
        return (x + d) % NX

    def py(d):
        return (y + d) % NY

    def bx(d):
        return (x + NX - d) % NX

    def by(d):
        return (y + NY - d) % NY

    def send(src, dst, ssem, rsem, to):
        pltpu.make_async_remote_copy(
            src_ref=src, dst_ref=dst, send_sem=ssem, recv_sem=rsem, device_id=to, device_id_type=MESH
        ).start()

    def done(ref, sem):
        pltpu.make_async_copy(ref, ref, sem).wait()

    def load_tokens(c):
        at = pl.ds(c * unit, unit)
        pltpu.make_async_copy(tok_hbm.at[at], tok.at[at], tok_sem.at[c]).start()

    def load_weights(g, h, sem):
        dy, dz = group_step(g)
        at = pl.multiple_of((((z + dz) % NZ) * NY + py(dy)) * cols, cols) + h * pair
        left, right = w.at[g, h, :, pl.ds(0, pair)], w.at[g, h, :, pl.ds(pair, pair)]
        pltpu.make_async_copy(kw_hbm.at[:, pl.ds(at, pair)], left, w_sem.at[sem]).start()
        pltpu.make_async_copy(vw_hbm.at[:, pl.ds(at, pair)], right, w_sem.at[sem]).start()

    def load_group(g):
        load_weights(g, 0, g)
        load_weights(g, 1, g)

    def tokens_here(c):
        done(tok.at[pl.ds(c * unit, unit)], tok_sem.at[c])

    load_weights(0, 0, 0)
    load_tokens(1)
    load_weights(1, 0, 1)
    load_tokens(0)
    load_weights(0, 1, GROUPS)
    load_tokens(2)

    barrier = pltpu.get_barrier_semaphore()
    peers = [dev(px(d), y, z) for d in NEAR] + [dev(x, py(d), z) for d in NEAR]
    peers += [dev(x, y, oz), (grp, sp, 1 - tp)]
    for p in peers:
        pl.semaphore_signal(barrier, inc=1, device_id=p, device_id_type=MESH)

    query = jnp.concatenate([q_ref[...].astype(F32), jnp.zeros((1, half), F32)], axis=-1)
    q8[...] = jnp.broadcast_to(query, q8.shape).astype(BF16)
    m_ref[...] = jnp.full(m_ref.shape, -1e30, F32)
    l_ref[...] = jnp.zeros(l_ref.shape, F32)
    a_ref[...] = jnp.zeros(a_ref.shape, F32)

    lane = lax.broadcasted_iota(jnp.int32, (unit, 2 * half), 1)

    def compute(*steps):
        made = []
        for g, h, c in steps:
            left = tok[c * unit : (c + 1) * unit, :]
            made.append(jnp.dot(left, w[g, h], preferred_element_type=F32))
        for (g, h, c), kv in zip(steps, made):
            dy, dz = group_step(g)
            yb, zb = py(dy), (z + dz) % NZ
            k, v = kv[:, :pair], kv[:, pair:]
            first = jnp.where(lane < half, k, pltpu.roll(v, half, 1)).astype(BF16)
            second = jnp.where(lane < half, pltpu.roll(k, half, 1), v).astype(BF16)
            for j, both in ((2 * h, first), (2 * h + 1, second)):
                if c == 0:
                    sr0[j + NX * (1 - ((j + NX - x) % NX + NX - 1) // NX), yb, zb] = both
                elif c == 1:
                    sr1[yb + NY * (1 - (dy + NY - 1) // NY), zb, j] = both
                else:
                    sr2[zb + NZ * (1 - dz), j, yb] = both

    def whole(g, c):
        compute((g, 0, c), (g, 1, c))

    def block(dy, dz):
        return (py(dy),) if dz is None else (py(dy), (z + dz) % NZ)

    def stop_x1(dy, dz):
        return (dy,) if dz is None else (dy, (z + dz) % NZ)

    def along_x(dy, dz):
        at = block(dy, dz)
        for d in (1, 3):
            send(sr0.at[(px(d), *at)], sr0.at[(NX + x, *at)], out_sem.at[0], r10.at[dy, d - 1], dev(px(d), y, z))
        s = WAY_X1[dy]
        stop = qx1.at[stop_x1(dy, dz)]
        send(sr0.at[(px(2), *at)], stop, out_sem.at[0], hx1.at[dy, dz or 0], dev(px(s), y, z))

    def relay_x1(dy, dz):
        s = WAY_X1[dy]
        stop = qx1.at[stop_x1(dy, dz)]
        done(stop, hx1.at[dy, dz or 0])
        send(stop, sr0.at[(NX + bx(s), *block(dy, dz))], hop_sem.at[0], r10.at[dy, 1], dev(px(s), y, z))

    def along_y(g, two=slice(None)):
        dy, dz = group_step(g)
        yb, zb = py(dy), (z + dz) % NZ
        send(sr1.at[yb, zb, two], sr1.at[NY + y, zb, two], out_sem.at[1], r11.at[dy - 1, dz], dev(x, yb, z))

    def start_y1(dz):
        to = dev(x, py(WAY_Y1[dz]), z)
        send(sr1.at[py(2), (z + dz) % NZ], qy1.at[dz], out_sem.at[1], hy1.at[dz], to)

    def relay_y1(dz):
        s = WAY_Y1[dz]
        done(qy1.at[dz], hy1.at[dz])
        send(qy1.at[dz], sr1.at[NY + by(s), (z + dz) % NZ], hop_sem.at[0], r11.at[1, dz], dev(x, py(s), z))

    def along_z(g):
        yb = py(group_step(g)[0])
        send(sr2.at[oz, :, yb], sr2.at[NZ + z, :, yb], out_sem.at[2], r12.at[0], dev(x, y, oz))

    done(w.at[0, 0], w_sem.at[0])
    tokens_here(1)
    done(w.at[1, 0], w_sem.at[1])
    load_weights(1, 1, GROUPS + 1)
    compute((0, 0, 1), (1, 0, 1))
    pl.semaphore_wait(barrier, len(peers))
    along_y(0, pl.ds(0, 2))
    along_y(1, pl.ds(0, 2))
    tokens_here(0)
    done(w.at[0, 1], w_sem.at[GROUPS])
    load_group(3)
    load_group(4)
    gate_loads = (
        pltpu.make_async_copy(gate_hbm, gin, gl_sem.at[0]),
        pltpu.make_async_copy(gate_hbm.at[:, :, x], gr.at[x], gl_sem.at[1]),
    )
    for load in gate_loads:
        load.start()
    whole(0, 0)
    along_x(1, 1)
    tokens_here(2)
    whole(0, 2)
    along_z(0)
    done(w.at[1, 1], w_sem.at[GROUPS + 1])
    whole(1, 0)
    along_x(3, 1)
    compute((0, 1, 1), (1, 1, 1))
    along_y(0, pl.ds(2, 2))
    along_y(1, pl.ds(2, 2))
    load_group(5)
    load_group(2)
    for load in gate_loads:
        load.wait()
    for d in NEAR:
        send(gin.at[:, :, px(d)], gr.at[x], gs_sem.at[0], gd_sem.at[0], dev(px(d), y, z))
    done(w.at[3], w_sem.at[3])
    whole(3, 0)
    along_x(3, 0)
    done(w.at[4], w_sem.at[4])
    whole(4, 1)
    start_y1(1)
    done(w.at[5], w_sem.at[5])
    whole(5, 1)
    start_y1(0)
    load_group(6)
    load_group(7)
    whole(1, 2)
    along_z(1)
    done(w.at[2], w_sem.at[2])
    whole(2, 0)
    along_x(1, 0)
    whole(2, 1)
    along_y(2)
    whole(3, 1)
    along_y(3)
    relay_x1(1, 1)
    relay_x1(3, 1)
    whole(4, 0)
    whole(5, 0)
    along_x(2, None)
    done(gr.at[0 : NX - 1], gd_sem.at[0])
    gt[y] = gr[:, :, y]
    for d in NEAR:
        send(gr.at[:, :, py(d)], gt.at[y], gs_sem.at[1], gd_sem.at[1], dev(x, py(d), z))
    whole(4, 2)
    along_z(4)
    done(w.at[6], w_sem.at[6])
    whole(6, 0)
    done(w.at[7], w_sem.at[7])
    whole(7, 0)
    along_x(0, None)
    relay_x1(3, 0)
    relay_x1(1, 0)
    whole(6, 2)
    along_z(6)
    whole(6, 1)
    whole(7, 1)
    whole(2, 2)
    relay_y1(1)
    relay_y1(0)
    whole(3, 2)
    whole(5, 2)
    whole(7, 2)

    def fwd0(dy, dx):
        src = sr0.at[NX + bx(dx), py(dy)]
        if dy == 2:
            send(src, qy2.at[dx], out_sem.at[0], hy2.at[dx], dev(x, py(WAY_Y[dx]), z))
        else:
            send(src, t0.at[y, bx(dx)], out_sem.at[0], r20.at[dy - 1], dev(x, py(dy), z))

    def relay_y2(dx):
        s = WAY_Y[dx]
        done(qy2.at[dx], hy2.at[dx])
        send(qy2.at[dx], t0.at[by(s), bx(dx)], hop_sem.at[1], r20.at[1], dev(x, py(s), z))

    def fwd1(dy):
        send(sr1.at[NY + by(dy), oz], t1.at[z, by(dy)], out_sem.at[1], r21.at[0], dev(x, y, oz))

    def fwd2(dx, dz):
        sz = (z + dz) % NZ
        src = sr2.at[NZ + sz, px(dx)]
        if dx == 2:
            send(src, qx2.at[dz], out_sem.at[2], hx2.at[dz], dev(px(WAY_X[dz]), y, z))
        else:
            send(src, t2.at[x, sz], out_sem.at[2], r22.at[dx - 1], dev(px(dx), y, z))

    def relay_x2(dz):
        s = WAY_X[dz]
        done(qx2.at[dz], hx2.at[dz])
        send(qx2.at[dz], t2.at[bx(s), (z + dz) % NZ], hop_sem.at[1], r22.at[1], dev(px(s), y, z))

    def got10(dy, dx):
        done(sr0.at[NX + bx(dx), py(dy)], r10.at[dy, dx - 1])

    def got11(dy, dz):
        done(sr1.at[NY + by(dy), (z + dz) % NZ], r11.at[dy - 1, dz])

    def got20(dy):
        done(t0.at[by(dy)], r20.at[dy - 1])

    def got22(dx):
        done(t2.at[bx(dx)], r22.at[dx - 1])

    def out0(dy):
        src = sr0.at[pl.ds(NX, NX), y, oz] if dy == 0 else t0.at[by(dy), :, oz]
        send(src, kv_ref.at[z, by(dy), :, 0], out_sem.at[0], r30.at[dy], dev(x, y, oz))

    def out1(dz, dx):
        sz = (z + dz) % NZ
        src = sr1.at[pl.ds(NY, NY), z, px(dx)] if dz == 0 else t1.at[sz, :, px(dx)]
        if dx == 2:
            send(src, qx3.at[dz], out_sem.at[1], hx3.at[dz], dev(px(WAY_X[dz]), y, z))
        else:
            send(src, kv_ref.at[sz, :, x, 1], out_sem.at[1], r31.at[dz, dx - 1], dev(px(dx), y, z))

    def relay_x3(dz):
        s = WAY_X[dz]
        done(qx3.at[dz], hx3.at[dz])
        send(qx3.at[dz], kv_ref.at[(z + dz) % NZ, :, bx(s), 1], hop_sem.at[2], r31.at[dz, 1], dev(px(s), y, z))

    def out2(dx, dy):
        src = sr2.at[pl.ds(NZ, NZ), x, py(dy)] if dx == 0 else t2.at[bx(dx), :, py(dy)]
        if dy == 2:
            send(src, qy3.at[dx], out_sem.at[2], hy3.at[dx], dev(x, py(WAY_Y[dx]), z))
        else:
            send(src, kv_ref.at[:, y, bx(dx), 2], out_sem.at[2], r32.at[dx, dy - 1], dev(x, py(dy), z))

    def relay_y3(dx):
        s = WAY_Y[dx]
        done(qy3.at[dx], hy3.at[dx])
        send(qy3.at[dx], kv_ref.at[:, by(s), bx(dx), 2], hop_sem.at[2], r32.at[dx, 1], dev(x, py(s), z))

    def keep0(dy):
        kv_ref[z, by(dy), :, 0] = sr0[NX : 2 * NX, y, z] if dy == 0 else t0[by(dy), :, z]

    def keep1(dz):
        sz = (z + dz) % NZ
        kv_ref[sz, :, x, 1] = sr1[NY : 2 * NY, z, x] if dz == 0 else t1[sz, :, x]

    def keep2(dx):
        kv_ref[:, y, bx(dx), 2] = sr2[NZ : 2 * NZ, x, y] if dx == 0 else t2[bx(dx), :, y]

    def come0(dy):
        done(kv_ref.at[oz, by(dy), :, 0], r30.at[dy])

    def come1(dz, dx):
        done(kv_ref.at[(z + dz) % NZ, :, bx(dx), 1], r31.at[dz, dx - 1])

    def come2(dx, dy):
        done(kv_ref.at[:, by(dy), bx(dx), 2], r32.at[dx, dy - 1])

    def part0(sz, sy):
        gates = [gate_ref[sz, sy, k, :, 0:unit] for k in range(NX)]
        return kv_ref[sz, sy, :, 0].reshape(NX * unit, 2 * half), gates

    def part1(sz, sx):
        gates = [gate_ref[sz, k, sx, :, unit : 2 * unit] for k in range(NY)]
        return kv_ref[sz, :, sx, 1].reshape(NY * unit, 2 * half), gates

    def part2(sy, sx):
        gates = [gate_ref[k, sy, sx, :, 2 * unit : 3 * unit] for k in range(NZ)]
        return kv_ref[:, sy, sx, 2].reshape(NZ * unit, 2 * half), gates

    def folded(op, values):
        width = 2 * half
        pieces = [v[:, i : i + width] for v in values for i in range(0, v.shape[1], width)]
        while len(pieces) > 1:
            pieces = [op(*pieces[i : i + 2]) if i + 1 < len(pieces) else pieces[i] for i in range(0, len(pieces), 2)]
        return pieces[0]

    def attend(parts):
        scores = []
        for kv, gates in parts:
            s = lax.dot_general(q8[...], kv, (((1,), (1,)), ((), ())), preferred_element_type=F32)
            scores.append(s * scale - jnp.concatenate(gates, axis=-1))
        old = m_ref[...]
        top = jnp.maximum(old, jnp.max(folded(jnp.maximum, scores), axis=1, keepdims=True))
        weights = [jnp.exp(s - top[:, :1]) for s in scores]
        keep = jnp.exp(old - top)
        m_ref[...] = top
        l_ref[...] = l_ref[...] * keep + jnp.sum(folded(jnp.add, weights), axis=1, keepdims=True)
        acc = a_ref[...] * keep
        for p, (kv, _) in zip(weights, parts):
            acc = acc + jnp.dot(p.astype(BF16), kv, preferred_element_type=F32)
        a_ref[...] = acc

    fwd1(0)
    fwd0(1, 0)
    fwd0(3, 0)
    fwd0(2, 0)
    for dy in (1, 3):
        got11(dy, 1)
        fwd1(dy)
    relay_x1(2, None)
    fwd2(2, 0)
    fwd2(1, 0)
    fwd2(3, 0)
    for dx in (1, 3):
        for dy in (1, 3, 2):
            got10(dy, dx)
            fwd0(dy, dx)
    for dy in (1, 3):
        got10(dy, 2)
        fwd0(dy, 2)
    relay_x1(0, None)
    done(gt.at[0 : NY - 1], gd_sem.at[1])
    send(gt.at[:, :, oz], gate_ref.at[z], gs_sem.at[2], gd_sem.at[2], dev(x, y, oz))
    gate_ref[z] = gt[:, :, z]
    got11(2, 1)
    fwd1(2)
    done(sr2.at[NZ + oz], r12.at[0])
    for dx in (2, 1, 3):
        fwd2(dx, 1)
    for dx in NEAR:
        got10(0, dx)
    out0(0)
    for dy in NEAR:
        got11(dy, 0)
    keep0(0)
    keep1(0)
    keep2(0)
    attend([part0(z, y), part1(z, x)])
    relay_x2(0)
    got10(2, 2)
    fwd0(2, 2)
    relay_y2(0)
    relay_y2(3)
    relay_y2(1)
    relay_x2(1)
    relay_y2(2)
    for d in (2, 1, 3):
        out1(0, d)
        out2(0, d)
    for dy in (1, 3):
        got20(dy)
        out0(dy)
    keep0(1)
    keep0(3)
    attend([part0(z, by(1)), part0(z, by(3))])
    for dx in (1, 3):
        got22(dx)
        for d in (2, dx, 4 - dx):
            out2(dx, d)
    got20(2)
    out0(2)
    done(t1.at[oz], r21.at[0])
    for d in (2, 3, 1):
        out1(1, d)
    got22(2)
    for d in (2, 3, 1):
        out2(2, d)
    relay_y3(0)
    keep0(2)
    keep1(1)
    for d in NEAR:
        keep2(d)
    done(gate_ref.at[oz], gd_sem.at[2])
    attend([part0(z, by(2)), part1(oz, x)] + [part2(y, bx(d)) for d in range(NX)])
    relay_x3(0)

    come0(0)
    come1(0, 3)
    for dx, dy in ((0, 3), (0, 1), (1, 3)):
        come2(dx, dy)
    attend([part0(oz, y), part1(z, bx(3)), part2(by(3), x), part2(by(1), x), part2(by(3), bx(1))])
    relay_y3(3)
    relay_y3(1)
    relay_x3(1)
    come0(1)
    come1(0, 1)
    for dx, dy in ((1, 1), (3, 3), (3, 1)):
        come2(dx, dy)
    attend([part0(oz, by(1)), part1(z, bx(1)), part2(by(1), bx(1)), part2(by(3), bx(3)), part2(by(1), bx(3))])
    relay_y3(2)
    come0(3)
    come1(1, 3)
    come2(2, 1)
    come2(2, 3)
    attend([part0(oz, by(3)), part1(oz, bx(3)), part2(by(1), bx(2)), part2(by(3), bx(2))])
    come1(1, 1)
    come2(0, 2)
    come2(3, 2)
    come2(1, 2)
    come2(2, 2)
    attend([part1(oz, bx(1))] + [part2(by(2), bx(d)) for d in range(NX)])
    come0(2)
    come1(0, 2)
    come1(1, 2)
    attend([part0(oz, by(2)), part1(z, bx(2)), part1(oz, bx(2))])

    stat[0:1, :] = m_ref[0:1, :]
    stat[1:2, :] = l_ref[0:1, :]
    stat[2:3, :] = a_ref[0:1, :]
    swap = pltpu.make_async_remote_copy(
        src_ref=stat, dst_ref=peer, send_sem=st.at[0], recv_sem=rt.at[0],
        device_id=(grp, sp, 1 - tp), device_id_type=MESH,
    )
    swap.start()
    done(sr0, out_sem.at[0])
    done(sr1, out_sem.at[1])
    done(sr2, out_sem.at[2])
    for k in range(3):
        done(t0.at[0:2], hop_sem.at[k])
    done(gr.at[0 : NX - 1], gs_sem.at[0])
    done(gt.at[0 : NY - 1], gs_sem.at[1])
    done(gate_ref.at[z], gs_sem.at[2])
    swap.wait()


def store_kernel(kv_ref, gate_ref, stat, peer, kv_out, gate_out, read_out, read_ref, sem):
    copies = [
        pltpu.make_async_copy(kv_ref.at[k, j], kv_out.at[k, j], sem.at[0]) for k in range(NZ) for j in range(NY)
    ]
    copies.append(pltpu.make_async_copy(gate_ref, gate_out, sem.at[1]))
    for c in copies:
        c.start()
    half = read_ref.shape[-1]
    tp = lax.axis_index("tp")
    first = jnp.where(tp == 0, stat[...], peer[...])
    second = jnp.where(tp == 0, peer[...], stat[...])
    top = jnp.maximum(first[0:1], second[0:1])
    e1, e2 = jnp.exp(first[0:1] - top), jnp.exp(second[0:1] - top)
    total = first[1:2] * e1 + second[1:2] * e2
    weighted = first[2:3] * e1 + second[2:3] * e2
    read_ref[0] = (weighted / total)[:, half:].astype(BF16)
    last = pltpu.make_async_copy(read_ref, read_out, sem.at[2])
    last.start()
    pltpu.make_async_copy(kv_ref, kv_out, sem.at[0]).wait()
    copies[-1].wait()
    last.wait()


def on_device(tokens, key_weight, value_weight, cum_gate, query):
    rows, width = tokens.shape[2:]
    hd = query.shape[2]
    unit = rows // COLORS
    cols = NX * hd
    kv_shape = (NZ, NY, NX, COLORS, unit, 2 * hd)
    gate_shape = (NZ, NY, NX, 1, rows)
    read_shape = (1, 1, hd)
    vmem = pl.BlockSpec(memory_space=pltpu.VMEM)
    anywhere = pl.BlockSpec(memory_space=pl.ANY)
    dma = pltpu.SemaphoreType.DMA
    u = (unit, 2 * hd)
    stat_shape = (8, 2 * hd)
    kv, gate, stat, peer = pl.pallas_call(
        exchange_kernel,
        out_shape=[
            pltpu.VMEM(kv_shape, BF16),
            pltpu.VMEM(gate_shape, F32),
            pltpu.VMEM(stat_shape, F32),
            pltpu.VMEM(stat_shape, F32),
        ],
        in_specs=[anywhere, anywhere, anywhere, anywhere, vmem],
        out_specs=[vmem, vmem, vmem, vmem],
        scratch_shapes=[
            pltpu.VMEM((rows, width), BF16),
            pltpu.VMEM((GROUPS, 2, width, cols), BF16),
            pltpu.VMEM((2 * NX, NY, NZ, *u), BF16),
            pltpu.VMEM((2 * NY, NZ, NX, *u), BF16),
            pltpu.VMEM((2 * NZ, NX, NY, *u), BF16),
            pltpu.VMEM((NY, NX, NZ, *u), BF16),
            pltpu.VMEM((NZ, NY, NX, *u), BF16),
            pltpu.VMEM((NX, NZ, NY, *u), BF16),
            pltpu.VMEM((NY, NZ, *u), BF16),
            pltpu.VMEM((NZ, NX, *u), BF16),
            pltpu.VMEM((NZ, NY, *u), BF16),
            pltpu.VMEM((NX, NZ, *u), BF16),
            pltpu.VMEM((NZ, NY, *u), BF16),
            pltpu.VMEM((NX, NZ, *u), BF16),
            pltpu.VMEM(gate_shape, F32),
            pltpu.VMEM((NX, NZ, NY, 1, rows), F32),
            pltpu.VMEM((NY, NX, NZ, 1, rows), F32),
            pltpu.VMEM((8, 2 * hd), BF16),
            pltpu.VMEM(stat_shape, F32),
            pltpu.VMEM(stat_shape, F32),
            pltpu.VMEM(stat_shape, F32),
            dma((COLORS,)), dma((GROUPS + 2,)), dma((2,)), dma((COLORS,)), dma((3,)), dma((3,)), dma((3,)),
            dma((NY, NZ)), dma((NZ,)), dma((NZ,)), dma((NX,)), dma((NZ,)), dma((NX,)),
            dma((NY, NX - 1)), dma((NY - 1, NZ)), dma((1,)),
            dma((NY - 1,)), dma((1,)), dma((NX - 1,)),
            dma((NY,)), dma((NZ, NX - 1)), dma((NX, NY - 1)), dma((1,)), dma((1,)),
        ],
        compiler_params=pltpu.CompilerParams(
            collective_id=0, has_side_effects=True, vmem_limit_bytes=50 * 2**20
        ),
        name="exchange",
    )(tokens.reshape(rows, width), key_weight, value_weight, cum_gate.reshape(gate_shape), query.reshape(1, hd))
    kv, gate, read = pl.pallas_call(
        store_kernel,
        out_shape=[
            jax.ShapeDtypeStruct(kv_shape, BF16),
            jax.ShapeDtypeStruct(gate_shape, F32),
            jax.ShapeDtypeStruct(read_shape, BF16),
        ],
        in_specs=[vmem] * 4,
        out_specs=[anywhere, anywhere, anywhere],
        scratch_shapes=[pltpu.VMEM(read_shape, BF16), dma((3,))],
        compiler_params=pltpu.CompilerParams(vmem_limit_bytes=2**20),
        name="store",
    )(kv, gate, stat, peer)
    length = NX * NY * NZ * rows
    return kv.reshape(1, 1, length, 2 * hd), gate.reshape(1, 1, length), read


def solution(mesh):
    placed = (P("gr", "tp", "sp", None), P(), P(), P("gr", None, "tp", "sp"), P("gr", "sp", None))
    return jax.shard_map(
        on_device,
        mesh=mesh,
        in_specs=placed,
        out_specs=(P("gr", "sp", "tp", None), P("gr", "sp", "tp"), P("gr", "sp", None)),
        check_vma=False,
    )
```
